128 devices in a mesh: kv: 16 (over z, y), tp: 8 (over x, core).
Axes of the slice: x: 4, y: 4, z: 4, core: 2. Of those that a mesh axis runs over, the one named last changes fastest.
Arguments:
- tokens: bfloat16 [2048, 4096], P(None, 'kv'), may hold values from -6 to 6
- norm_gain: float32 [4096], replicated, may hold values from 0.1 to 1.9
- query_weight: bfloat16 [4096, 2048], P('kv', 'tp'), may hold values from -0.09375 to 0.09375
- key_weight: bfloat16 [4096, 2048], P('kv', 'tp'), may hold values from -0.09375 to 0.09375
- value_weight: bfloat16 [4096, 4096], P('kv', 'tp'), may hold values from -0.09375 to 0.09375
- outgate_weight: bfloat16 [4096, 4096], P('kv', 'tp'), may hold values from -0.09375 to 0.09375
- gate_weight: bfloat16 [4096, 32], P('kv'), may hold values from -0.09375 to 0.09375
- forget_bias: float32 [16], replicated, may hold values from -1 to 5
- head_gain: float32 [4096], P('tp'), may hold values from 0.1 to 1.9
- output_weight: bfloat16 [4096, 4096], P('tp', 'kv'), may hold values from -0.09375 to 0.09375
- state_matrix: float32 [512, 16, 128, 256], P('kv', 'tp'), may hold values from -6 to 6
- state_normal: float32 [512, 16, 128], P('kv', 'tp'), may hold values from -6 to 6
- state_stable: float32 [512, 16], P('kv', 'tp'), may hold values from -3 to 3
- prior_keys: bfloat16 [512, 4, 2048], P('kv', None, 'tp'), may hold values from -0.59765625 to 0.59765625
- prior_values: bfloat16 [512, 4, 4096], P('kv', None, 'tp'), may hold values from -6 to 6
- prior_ingate: float32 [512, 4, 16], P('kv', None, 'tp'), may hold values from -4 to 4
- prior_forget: float32 [512, 4, 16], P('kv', None, 'tp'), may hold values from -2 to -0.02
- accepted: int32 [512], P('kv'), may hold values from 0 to 4
- parents: int32 [512, 4], P('kv'), may hold values from -1 to 2, as said below
Outputs:
- layer_out: bfloat16 [2048, 4096], P('tp', 'kv')
- new_matrix: float32 [512, 16, 128, 256], P('kv', 'tp')
- new_normal: float32 [512, 16, 128], P('kv', 'tp')
- new_stable: float32 [512, 16], P('kv', 'tp')
The draws below stay inside these ranges and needn't reach their ends.
Inputs may be any that keep to these rules, and one draw needn't show every extreme that they name: parents of proposal t lie in -1 to t - 1; the first proposal's parent is -1; in some sequence each proposal's parent is the one before it.
All inputs are finite; a program needn't handle non-finite values.
Results may differ from the reference program's by a relative error of at most 0.0089.
Values may be sent and summed in bfloat16 or wider, within the bound.
A program may use at most 128 MiB of HBM per device.

```python
import jax
import jax.numpy as jnp
from jax import lax

D = 4096
HEADS = 16
DQK = 128
DV = 256
PROP = 4
SEQS = 512
TOKENS = 2048


def draw_parents(key, part):
    random_ints = jax.random.randint(key, (SEQS, PROP), 0, 1 << 20)
    position = jnp.arange(PROP, dtype=jnp.int32)[None, :]
    chosen = random_ints % jnp.maximum(position, 1)
    leading = jnp.arange(SEQS, dtype=jnp.int32)[:, None] == 0
    chosen = jnp.where(leading, position - 1, chosen)
    return jnp.where(position == 0, -1, chosen).astype(jnp.int32)


def set_ends(entries, rng, least, top_value):
    dims = entries.shape
    place = [jax.random.randint(jax.random.fold_in(rng, axis), (), 0, dims[axis]) for axis in range(len(dims))]
    entries = entries.at[tuple(place)].set(least)
    longest = dims.index(max(dims))
    place[longest] = (place[longest] + 1) % dims[longest]
    return entries.at[tuple(place)].set(top_value)


def block_scale(rng, shape, shards, least, largest):
    def one(axis_at, parts):
        steps = jax.random.uniform(jax.random.fold_in(jax.random.fold_in(rng, 6), axis_at), (parts,), jnp.float32, least / len(shards), largest / len(shards))
        return jnp.repeat(jnp.exp(steps), shape[axis_at] // parts).reshape((-1,) + (1,) * (len(shape) - axis_at - 1))

    factor_of = one(*shards[0])
    for cut in shards[1:]:
        factor_of = factor_of * one(*cut)
    return factor_of


def centred(rng, dims, scale, most, shards=(), kind=jnp.bfloat16):
    loudness = block_scale(rng, dims, shards, -0.22, 0.18) if shards else 1.0
    array = jax.random.normal(rng, dims, jnp.float32) * scale * loudness
    return jnp.minimum(jnp.maximum(array, -most), most).astype(kind)


def setup_inputs(seed: int = 0) -> dict:
    keys = jax.random.split(jax.random.key(seed), 20)
    return {
        "tokens": centred(keys[0], (TOKENS, D), 1.0, 6.0, ((1, 16),)),
        "norm_gain": jnp.clip(1.0 + 0.18 * jax.random.normal(keys[1], (D,), jnp.float32), 0.1, 1.9),
        "query_weight": centred(keys[2], (D, HEADS * DQK), D ** -0.5, 0.09375, ((0, 16), (1, 8))),
        "key_weight": centred(keys[3], (D, HEADS * DQK), D ** -0.5, 0.09375, ((0, 16), (1, 8))),
        "value_weight": centred(keys[4], (D, HEADS * DV), D ** -0.5, 0.09375, ((0, 16), (1, 8))),
        "outgate_weight": centred(keys[5], (D, HEADS * DV), D ** -0.5, 0.09375, ((0, 16), (1, 8))),
        "gate_weight": centred(keys[6], (D, 2 * HEADS), D ** -0.5, 0.09375, ((0, 16),)),
        "forget_bias": jnp.clip(jax.random.uniform(keys[7], (HEADS,), jnp.float32, -1.0, 5.0), -1.0, 5.0),
        "head_gain": jnp.clip(1.0 + 0.18 * jax.random.normal(keys[8], (HEADS * DV,), jnp.float32), 0.1, 1.9),
        "output_weight": centred(keys[9], (HEADS * DV, D), (HEADS * DV) ** -0.5, 0.09375, ((0, 8), (1, 16))),
        "state_matrix": centred(keys[10], (SEQS, HEADS, DQK, DV), 1.0, 6.0, ((0, 16), (1, 8)), jnp.float32),
        "state_normal": centred(keys[11], (SEQS, HEADS, DQK), 1.0, 6.0, ((0, 16), (1, 8)), jnp.float32),
        "state_stable": centred(keys[12], (SEQS, HEADS), 1.0, 3.0, ((0, 16), (1, 8)), jnp.float32),
        "prior_keys": centred(keys[13], (SEQS, PROP, HEADS * DQK), 0.09, 0.59765625, ((0, 16), (2, 8))),
        "prior_values": centred(keys[14], (SEQS, PROP, HEADS * DV), 1.0, 6.0, ((0, 16), (2, 8))),
        "prior_ingate": centred(keys[15], (SEQS, PROP, HEADS), 1.0, 4.0, ((0, 16), (2, 8)), jnp.float32),
        "prior_forget": jnp.clip(-2.0 + 1.98 * jax.random.uniform(keys[16], (SEQS, PROP, HEADS), jnp.float32) ** block_scale(keys[16], (SEQS, PROP, HEADS), ((0, 16), (2, 8)), -0.2, 0.2), -2.0, -0.02),
        "accepted": set_ends(jax.random.randint(keys[17], (SEQS,), 0, PROP + 1), jax.random.fold_in(keys[17], 1), 0, PROP).astype(jnp.int32),
        "parents": draw_parents(jax.random.fold_in(keys[19], 71), 0),
    }


def ancestry(parents):
    count = parents.shape[1]
    index = jnp.arange(count, dtype=jnp.int32)
    current = jnp.broadcast_to(index[None, :], parents.shape).astype(jnp.int32)
    table = jnp.broadcast_to((index[:, None] == index[None, :]).astype(jnp.float32), (parents.shape[0], count, count))
    for repeat in range(count - 1):
        looked = jnp.take_along_axis(parents, jnp.maximum(current, 0), axis=1)
        current = jnp.where(current >= 0, looked, -1).astype(jnp.int32)
        table = table + (current[:, :, None] == index[None, None, :]).astype(jnp.float32)
    return table

def commit(matrix, normal, stable, prior_k, prior_v, prior_i, prior_f, accepted):
    count = prior_k.shape[1]
    live = (jnp.arange(count, dtype=jnp.int32)[None, :] < accepted[:, None])[:, :, None]
    forget_live = jnp.where(live, prior_f, 0.0)
    cumul = jnp.cumsum(forget_live, axis=1)
    total = cumul[:, -1]
    weight_log = jnp.where(live, total[:, None, :] - cumul + prior_i, -jnp.inf)
    new_stable = jnp.maximum(total + stable, lax.optimization_barrier(jnp.max(weight_log, axis=1)))
    weights = jnp.exp(weight_log - new_stable[:, None, :])
    decay = jnp.exp(total + stable - new_stable)
    hp = lax.Precision.HIGHEST
    new_matrix = decay[:, :, None, None] * matrix + jnp.einsum('sph,sphd,sphv->shdv', weights, prior_k, prior_v, precision=hp)
    new_normal = decay[:, :, None] * normal + jnp.einsum('sph,sphd->shd', weights, prior_k, precision=hp)
    return (new_matrix, new_normal, new_stable)

def tree_read(query, key_rows, value_rows, ingate, logforget, table, matrix, normal, stable):
    hp = lax.Precision.HIGHEST
    path_sum = jnp.einsum('sta,sah->sth', table, logforget, precision=hp)
    dlog = path_sum[:, :, None, :] - path_sum[:, None, :, :] + ingate[:, None, :, :]
    dlog = jnp.where(table[:, :, :, None] > 0.5, dlog, -jnp.inf)
    carried = path_sum + stable[:, None, :]
    top = jnp.maximum(carried, lax.optimization_barrier(jnp.max(dlog, axis=2)))
    scores = jnp.einsum('sthd,sahd->stah', query, key_rows, precision=hp) * jnp.exp(dlog - top[:, :, None, :])
    factor = jnp.exp(carried - top)
    numer = jnp.einsum('stah,sahv->sthv', scores, value_rows, precision=hp) + factor[..., None] * jnp.einsum('sthd,shdv->sthv', query, matrix, precision=hp)
    denom = lax.optimization_barrier(jnp.sum(scores, axis=2)) + factor * jnp.einsum('sthd,shd->sth', query, normal, precision=hp)
    return numer / jnp.maximum(jnp.abs(denom), jnp.exp(-top))[..., None]

def reference(tokens, norm_gain, query_weight, key_weight, value_weight, outgate_weight, gate_weight, forget_bias, head_gain, output_weight, state_matrix, state_normal, state_stable, prior_keys, prior_values, prior_ingate, prior_forget, accepted, parents):
    f32 = jnp.float32
    xfloat = tokens.astype(f32)
    scale = lax.rsqrt(lax.optimization_barrier(jnp.sum(xfloat * xfloat, axis=-1, keepdims=True)) / D + 1e-06)
    normed = (xfloat * norm_gain).astype(jnp.bfloat16)
    query = scale * jnp.dot(normed, query_weight, preferred_element_type=f32)
    key_rows = scale * jnp.dot(normed, key_weight, preferred_element_type=f32) / jnp.sqrt(jnp.float32(DQK))
    value_rows = scale * jnp.dot(normed, value_weight, preferred_element_type=f32)
    outgate = scale * jnp.dot(normed, outgate_weight, preferred_element_type=f32)
    gates = scale * jnp.dot(normed, gate_weight, preferred_element_type=f32)
    ingate = gates[:, :HEADS].reshape(SEQS, PROP, HEADS)
    logforget = jax.nn.log_sigmoid(gates[:, HEADS:] + forget_bias).reshape(SEQS, PROP, HEADS)
    new_matrix, new_normal, new_stable = commit(state_matrix, state_normal, state_stable, prior_keys.astype(f32).reshape(SEQS, PROP, HEADS, DQK), prior_values.astype(f32).reshape(SEQS, PROP, HEADS, DV), prior_ingate, prior_forget, accepted)
    table = ancestry(parents)
    read = tree_read(query.reshape(SEQS, PROP, HEADS, DQK), key_rows.reshape(SEQS, PROP, HEADS, DQK), value_rows.reshape(SEQS, PROP, HEADS, DV), ingate, logforget, table, new_matrix, new_normal, new_stable)
    normer = lax.rsqrt(lax.optimization_barrier(jnp.mean(read * read, axis=-1, keepdims=True)) + 1e-06)
    hidden = read * normer * head_gain.reshape(HEADS, DV) * jax.nn.sigmoid(outgate.reshape(SEQS, PROP, HEADS, DV))
    hidden = hidden.reshape(TOKENS, HEADS * DV).astype(jnp.bfloat16)
    layer_out = jnp.dot(hidden, output_weight, preferred_element_type=f32).astype(jnp.bfloat16)
    return (layer_out, new_matrix, new_normal, new_stable)
```

```python
import functools

import jax
import jax.numpy as jnp
from jax import lax
from jax.experimental import pallas as pl
from jax.experimental.pallas import tpu as pltpu
from jax.sharding import Mesh
from jax.sharding import PartitionSpec as P

D = 4096
HEADS = 16
DQK = 128
DV = 256
PROP = 4
KV = ("z", "y")
TP = ("x", "c")
RING = 4
BLOCK = 128
WIDE = 256
UNITS = 6
MESH = pl.DeviceIdType.MESH
f32 = jnp.float32
bf16 = jnp.bfloat16
NEG = -1e30


def ring_of(axis):
    me = lax.axis_index(axis)
    return me, lax.rem(me + 1, RING), lax.rem(me + RING - 1, RING), lax.rem(me + 2, RING)


def iota(shape, dim):
    return lax.broadcasted_iota(jnp.int32, shape, dim)


def meet(peers):
    barrier = pltpu.get_barrier_semaphore()
    for peer in peers:
        pl.semaphore_signal(barrier, inc=1, device_id=peer, device_id_type=MESH)
    pl.semaphore_wait(barrier, len(peers))


def send(src, dst, ssem, rsem, peer):
    copy = pltpu.make_async_remote_copy(
        src_ref=src, dst_ref=dst, send_sem=ssem, recv_sem=rsem, device_id=peer, device_id_type=MESH
    )
    copy.start()
    return copy


def project_kernel(
    x_ref, gain_ref, wq_ref, wk_ref, wv_ref, wo_ref, wg_ref, y_ref, g_ref,
    normed, m1, m2, dep, m3, own, r1, r2, r3, n1, n2, n3, q1, q2, q3,
    gall, gin, gsum, gin2, ssem, rsem, gssem, grsem,
):
    rings = {"z": ring_of("z"), "y": ring_of("y")}
    meet([{a: rings[a][k]} for a in ("z", "y") for k in (1, 2, 3)])
    me_kv = rings["z"][0] * RING + rings["y"][0]
    gain = gain_ref[pl.ds(2 * me_kv, 2), :]
    gain = jnp.concatenate([gain[0:1], gain[1:2]], axis=1)

    def norm_block(k, carry):
        normed[k] = (x_ref[pl.ds(pl.multiple_of(k * BLOCK, BLOCK), BLOCK), :].astype(f32) * gain).astype(bf16)
        return carry

    lax.fori_loop(0, RING * RING, norm_block, 0)

    def rows_of(axis, group):
        if axis == "z":
            part = normed[pl.ds(group * RING, RING)]
        else:
            part = jnp.concatenate([normed[pl.ds(k * RING + group, 1)] for k in range(RING)], axis=0)
        return part.reshape(RING * BLOCK, WIDE)

    def weight(unit):
        lane, c = divmod(unit, 3)
        if lane == 0:
            return (wq_ref[...], wk_ref[...], wo_ref[:, :WIDE])[c]
        return (wv_ref[:, :WIDE], wv_ref[:, WIDE:], wo_ref[:, WIDE:])[c]

    def out_cols(unit):
        lane, c = divmod(unit, 3)
        at = ((0, 256, 1024) if lane == 0 else (512, 768, 1280))[c]
        return slice(at, at + WIDE)

    axes_of = lambda unit: ("z", "y") if unit < 3 else ("y", "z")
    sent = []
    arrived = {}
    half = RING * BLOCK // 2

    def ship(stage, unit, kind, way, src, dst):
        axis = axes_of(unit)[stage]
        slot = ((stage * UNITS + unit) * 3 + kind) * 2 + way
        copy = send(src, dst, ssem.at[slot], rsem.at[slot], {axis: rings[axis][1 + way]})
        sent.append(copy)
        arrived[(stage, unit, kind, way)] = copy

    order = [0, 3, 1, 4, 2, 5]
    for unit in order:
        axis = axes_of(unit)[0]
        me, nxt, prv, opp = rings[axis]
        w = weight(unit)
        part = jnp.dot(rows_of(axis, opp), w, preferred_element_type=f32).astype(bf16)
        m1[unit, 0] = part[:half]
        m1[unit, 1] = part[half:]
        ship(0, unit, 0, 0, m1.at[unit, 0], r1.at[unit, 0])
        ship(0, unit, 0, 1, m1.at[unit, 1], r1.at[unit, 1])
        part = jnp.dot(rows_of(axis, nxt), w, preferred_element_type=f32)
        dep[unit, 0] = part[:half]
        m2[unit, 0] = part[half:].astype(bf16)
        ship(0, unit, 1, 0, m2.at[unit, 0], r2.at[unit, 0])
        part = jnp.dot(rows_of(axis, prv), w, preferred_element_type=f32)
        dep[unit, 1] = part[half:]
        m2[unit, 1] = part[:half].astype(bf16)
        ship(0, unit, 1, 1, m2.at[unit, 1], r2.at[unit, 1])
        own[unit] = jnp.dot(rows_of(axis, me), w, preferred_element_type=f32).reshape(RING, BLOCK, WIDE)

    tp_at = lax.axis_index("x") * 2 + lax.axis_index("c")
    row = iota((8, 32), 0)
    col = iota((8, 32), 1)
    pick = jnp.where(row < 2, 2 * tp_at + row, jnp.where(row < 4, HEADS + 2 * tp_at + row - 2, -1))
    wg = jnp.dot((pick == col).astype(bf16), wg_ref[...], preferred_element_type=f32).astype(bf16)
    ones = (iota((8, WIDE), 0) == 4).astype(bf16)
    lanes = (((1,), (1,)), ((), ()))
    for group in range(RING):
        xs = x_ref[group * 512 : (group + 1) * 512, :].astype(f32)
        squares = xs * xs
        high = squares.astype(bf16)
        low = (squares - high.astype(f32)).astype(bf16)
        tile = lax.dot_general(wg, normed[group * RING : (group + 1) * RING].reshape(512, WIDE), lanes, preferred_element_type=f32)
        tile += lax.dot_general(ones, high, lanes, preferred_element_type=f32)
        tile += lax.dot_general(ones, low, lanes, preferred_element_type=f32)
        gall[group] = tile
    gates1 = []
    for k in (1, 2, 3):
        peer = rings["z"][k]
        gates1.append(send(gall.at[peer], gin.at[k - 1], gssem.at[k - 1], grsem.at[k - 1], {"z": peer}))

    def finish_first(unit):
        axis = axes_of(unit)[0]
        for way in range(2):
            arrived[(0, unit, 0, way)].wait_recv()
            m3[unit, way] = (dep[unit, way] + r1[unit, way].astype(f32)).astype(bf16)
            ship(0, unit, 2, way, m3.at[unit, way], r3.at[unit, way])

    for unit in order:
        finish_first(unit)

    for copy in gates1:
        copy.wait_recv()
    total = gall[rings["z"][0]] + gin[0] + gin[1] + gin[2]
    for k in range(RING):
        gsum[k] = total[:, k * BLOCK : (k + 1) * BLOCK]
    gates2 = []
    for k in (1, 2, 3):
        peer = rings["y"][k]
        gates2.append(send(gsum.at[peer], gin2.at[k - 1], gssem.at[k + 2], grsem.at[k + 2], {"y": peer}))

    quarter = BLOCK // 2
    for unit in order:
        axis = axes_of(unit)[1]
        me, nxt, prv, opp = rings[axis]
        for way in range(2):
            arrived[(0, unit, 1, way)].wait_recv()
            arrived[(0, unit, 2, way)].wait_recv()
        low = own[unit, 0:2].reshape(half, WIDE) + r3[unit, 0].astype(f32) + r2[unit, 1].astype(f32)
        high = own[unit, 2:4].reshape(half, WIDE) + r2[unit, 0].astype(f32) + r3[unit, 1].astype(f32)
        own[unit, 0:2] = low.reshape(2, BLOCK, WIDE)
        own[unit, 2:4] = high.reshape(2, BLOCK, WIDE)
        n1[unit, 0] = own[unit, opp, :quarter].astype(bf16)
        n1[unit, 1] = own[unit, opp, quarter:].astype(bf16)
        ship(1, unit, 0, 0, n1.at[unit, 0], q1.at[unit, 0])
        ship(1, unit, 0, 1, n1.at[unit, 1], q1.at[unit, 1])
        n2[unit, 0] = own[unit, nxt, quarter:].astype(bf16)
        ship(1, unit, 1, 0, n2.at[unit, 0], q2.at[unit, 0])
        n2[unit, 1] = own[unit, prv, :quarter].astype(bf16)
        ship(1, unit, 1, 1, n2.at[unit, 1], q2.at[unit, 1])

    for unit in order:
        axis = axes_of(unit)[1]
        me, nxt, prv, opp = rings[axis]
        arrived[(1, unit, 0, 0)].wait_recv()
        n3[unit, 0] = (own[unit, nxt, :quarter] + q1[unit, 0].astype(f32)).astype(bf16)
        ship(1, unit, 2, 0, n3.at[unit, 0], q3.at[unit, 0])
        arrived[(1, unit, 0, 1)].wait_recv()
        n3[unit, 1] = (own[unit, prv, quarter:] + q1[unit, 1].astype(f32)).astype(bf16)
        ship(1, unit, 2, 1, n3.at[unit, 1], q3.at[unit, 1])

    for copy in gates2:
        copy.wait_recv()
    g_ref[...] = gsum[rings["y"][0]] + gin2[0] + gin2[1] + gin2[2]

    for unit in order:
        me = rings[axes_of(unit)[1]][0]
        for way in range(2):
            arrived[(1, unit, 1, way)].wait_recv()
            arrived[(1, unit, 2, way)].wait_recv()
        cols = out_cols(unit)
        y_ref[:quarter, cols] = own[unit, me, :quarter] + q3[unit, 0].astype(f32) + q2[unit, 1].astype(f32)
        y_ref[quarter:, cols] = own[unit, me, quarter:] + q2[unit, 0].astype(f32) + q3[unit, 1].astype(f32)

    for copy in sent + gates1 + gates2:
        copy.wait_send()


def project(tokens, norm_gain, query_weight, key_weight, value_weight, outgate_weight, gate_weight):
    vmem = pl.BlockSpec(memory_space=pltpu.VMEM)
    first = lambda kind: pltpu.VMEM((UNITS, 2, 256, WIDE), kind)
    second = pltpu.VMEM((UNITS, 2, 64, WIDE), bf16)
    return pl.pallas_call(
        project_kernel,
        out_shape=(jax.ShapeDtypeStruct((BLOCK, 1536), f32), jax.ShapeDtypeStruct((8, BLOCK), f32)),
        in_specs=[vmem] * 7,
        out_specs=(vmem, vmem),
        scratch_shapes=[
            pltpu.VMEM((16, BLOCK, WIDE), bf16),
            first(bf16), first(bf16), first(f32), first(bf16),
            pltpu.VMEM((UNITS, RING, BLOCK, WIDE), f32),
            first(bf16), first(bf16), first(bf16),
            second, second, second, second, second, second,
            pltpu.VMEM((RING, 8, 512), f32),
            pltpu.VMEM((3, 8, 512), f32),
            pltpu.VMEM((RING, 8, BLOCK), f32),
            pltpu.VMEM((3, 8, BLOCK), f32),
            pltpu.SemaphoreType.DMA((72,)),
            pltpu.SemaphoreType.DMA((72,)),
            pltpu.SemaphoreType.DMA((6,)),
            pltpu.SemaphoreType.DMA((6,)),
        ],
        compiler_params=pltpu.CompilerParams(
            collective_id=0, has_side_effects=True, vmem_limit_bytes=50 * 1024 * 1024
        ),
        cost_estimate=pl.CostEstimate(flops=2 * 2048 * 256 * 1540, bytes_accessed=3_000_000, transcendentals=0),
        name="project",
    )(tokens, norm_gain.reshape(32, 128), query_weight, key_weight, value_weight, outgate_weight, gate_weight.T)


def to_col(row, eye):
    return jnp.sum(jnp.where(eye, row, 0.0), axis=1, keepdims=True)


def to_row(col, eye):
    return jnp.sum(jnp.where(eye, col, 0.0), axis=0, keepdims=True)


SEQ_STEP = 4


def cell_kernel(
    bias_ref, y_ref, g_ref, pk_ref, pv_ref, pi_ref, pf_ref, acc_ref, par_ref, stable_ref, gain_ref, normal_ref, state_ref,
    hidden_ref, state_out, normal_out, stable_out,
    kt, wv, decay, qs, mem, nsrow,
):
    step = pl.program_id(0)
    heads = 2
    eye = iota((BLOCK, BLOCK), 0) == iota((BLOCK, BLOCK), 1)
    seq_of = iota((BLOCK, 32), 0) // PROP == iota((BLOCK, 32), 1)
    place = iota((BLOCK, 32), 0) % PROP

    def spread(rows):
        picked = jnp.broadcast_to(rows[0], (BLOCK, 32))
        for p in range(1, PROP):
            picked = jnp.where(place == p, rows[p], picked)
        return jnp.sum(jnp.where(seq_of, picked, 0.0), axis=1, keepdims=True)

    @pl.when(step == 0)
    def _():
        acc = acc_ref[...].astype(f32)
        live = [acc > p for p in range(PROP)]
        forget = [jnp.where(live[p], pf_ref[p], 0.0) for p in range(PROP)]
        cum = [forget[0]]
        for p in range(1, PROP):
            cum.append(cum[-1] + forget[p])
        total = cum[-1]
        logs = [jnp.where(live[p], total - cum[p] + pi_ref[p], NEG) for p in range(PROP)]
        carried = total + stable_ref[...]
        new_stable = carried
        for p in range(PROP):
            new_stable = jnp.maximum(new_stable, logs[p])
        stable_out[...] = new_stable
        weights = [jnp.where(live[p], jnp.exp(logs[p] - new_stable), 0.0) for p in range(PROP)]
        fade = jnp.exp(carried - new_stable)
        scale_col = to_col(lax.rsqrt(g_ref[4:5] / D + 1e-6), eye)
        seq_pick = iota((32, BLOCK), 0) == iota((32, BLOCK), 1) // PROP
        eye32 = iota((32, 32), 0) == iota((32, 32), 1)
        for h in range(heads):
            wcol = spread([weights[p][h : h + 1] for p in range(PROP)])
            keys = pk_ref[:, h * DQK : (h + 1) * DQK].astype(f32)
            kt[h] = keys.T.astype(bf16)
            wv[h] = (wcol * pv_ref[:, h * DV : (h + 1) * DV].astype(f32)).astype(bf16)
            fcol = jnp.sum(jnp.where(eye32, fade[h : h + 1], 0.0), axis=1, keepdims=True)
            decay[h] = jnp.broadcast_to(fcol, (32, DQK))
            summed = jnp.dot(seq_pick.astype(f32), wcol * keys, preferred_element_type=f32, precision=lax.Precision.HIGHEST)
            new_normal = fcol * normal_ref[:, h, :] + summed
            normal_out[:, h, :] = new_normal
            qs[h] = y_ref[:, h * DQK : (h + 1) * DQK] * scale_col
            nsrow[h] = jnp.broadcast_to(spread([new_stable[h : h + 1]] * PROP), (BLOCK, DQK))

    even = iota((8, DQK), 0) < PROP
    prior_seq = iota((BLOCK, DV), 0) // PROP
    for h in range(heads):
        for pair in range(SEQ_STEP // 2):
            tiles = []
            for k in range(2):
                j = pair * 2 + k
                s = step * SEQ_STEP + j
                rhs = jnp.where(prior_seq == s, wv[h].astype(f32), 0.0).astype(bf16)
                fresh = jnp.dot(kt[h], rhs, preferred_element_type=f32)
                d = decay[h, pl.ds(s, 1), :]
                d = jnp.concatenate([d, d], axis=1)
                tile = d * state_ref[j, h] + fresh
                state_out[j, h] = tile
                tiles.append(tile.astype(bf16))
            at = pl.multiple_of((step * SEQ_STEP + pair * 2) * PROP, 8)
            q8 = qs[h, pl.ds(at, 8), :]
            lhs = jnp.concatenate([jnp.where(even, q8, 0.0), jnp.where(even, 0.0, q8)], axis=1)
            high = lhs.astype(bf16)
            both = jnp.concatenate([high.astype(f32), lhs - high.astype(f32)], axis=0).astype(bf16)
            got = jnp.dot(both, jnp.concatenate(tiles, axis=0), preferred_element_type=f32)
            mem[h, pl.ds(at, 8), :] = got[:8] + got[8:]

    @pl.when(step == pl.num_programs(0) - 1)
    def _():
        scale_row = lax.rsqrt(g_ref[4:5] / D + 1e-6)
        scale_col = to_col(scale_row, eye)
        parent = spread([par_ref[p : p + 1].astype(f32) for p in range(PROP)])
        base = (iota((BLOCK, 1), 0) // PROP * PROP).astype(f32)
        goal = jnp.where(parent < 0, -1.0, parent + base)
        up = (iota((BLOCK, BLOCK), 1).astype(f32) == goal).astype(f32)
        upb = up.astype(bf16)
        up2 = jnp.dot(upb, upb, preferred_element_type=f32)
        up3 = jnp.dot(up2.astype(bf16), upb, preferred_element_type=f32)
        path = (eye.astype(f32) + up + up2 + up3) > 0.5
        for h in range(heads):
            bias = bias_ref[0, h]
            ingate = scale_row * g_ref[h : h + 1]
            logforget = jax.nn.log_sigmoid(scale_row * g_ref[2 + h : 3 + h] + bias)
            b_col = jnp.sum(jnp.where(path, logforget, 0.0), axis=1, keepdims=True)
            b_row = to_row(b_col, eye)
            dlog = jnp.where(path, b_col - b_row + ingate, NEG)
            ns = nsrow[h]
            carried = b_col + ns[:, 0:1]
            top = jnp.maximum(carried, jnp.max(dlog, axis=1, keepdims=True))
            query = qs[h]
            keys = y_ref[:, 256 + h * DQK : 256 + (h + 1) * DQK] * (scale_col * DQK**-0.5)
            values = y_ref[:, 512 + h * DV : 512 + (h + 1) * DV] * scale_col
            outgate = y_ref[:, 1024 + h * DV : 1024 + (h + 1) * DV] * scale_col
            dots = lax.dot_general(
                query, keys, (((1,), (1,)), ((), ())), preferred_element_type=f32, precision=lax.Precision.HIGHEST
            )
            scores = dots * jnp.where(path, jnp.exp(dlog - top), 0.0)
            factor = jnp.exp(carried - top)
            numer = jnp.dot(scores, values, preferred_element_type=f32, precision=lax.Precision.HIGHEST) + factor * mem[h]
            normal = jnp.dot(
                seq_of.astype(f32), normal_out[:, h, :], preferred_element_type=f32, precision=lax.Precision.HIGHEST
            )
            denom = jnp.sum(scores, axis=1, keepdims=True) + factor * jnp.sum(query * normal, axis=1, keepdims=True)
            read = numer / jnp.maximum(jnp.abs(denom), jnp.exp(-top))
            mean = jnp.sum(read * read, axis=1, keepdims=True) / DV
            gain = gain_ref[:, h * DV : (h + 1) * DV]
            hidden = read * lax.rsqrt(mean + 1e-6) * gain * jax.nn.sigmoid(outgate)
            hidden_ref[:, h * DV : (h + 1) * DV] = hidden.astype(bf16)


def cell(y, g, bias, prior_keys, prior_values, prior_ingate, prior_forget, accepted, parents, stable, gain, normal, state):
    whole = lambda a: pl.BlockSpec(a.shape, lambda i: (0,) * a.ndim)
    small = [
        y, g, prior_keys.reshape(BLOCK, 256), prior_values.reshape(BLOCK, 512),
        prior_ingate.transpose(1, 2, 0), prior_forget.transpose(1, 2, 0),
        accepted.reshape(1, 32), parents.T, stable.T, gain.reshape(1, 512), normal,
    ]
    block = pl.BlockSpec((SEQ_STEP, 2, DQK, DV), lambda i: (i, 0, 0, 0))
    hidden, new_matrix, new_normal, new_stable = pl.pallas_call(
        cell_kernel,
        grid=(32 // SEQ_STEP,),
        out_shape=(
            jax.ShapeDtypeStruct((BLOCK, 512), bf16),
            jax.ShapeDtypeStruct((32, 2, DQK, DV), f32),
            jax.ShapeDtypeStruct((32, 2, DQK), f32),
            jax.ShapeDtypeStruct((2, 32), f32),
        ),
        in_specs=[pl.BlockSpec(memory_space=pltpu.SMEM)] + [whole(a) for a in small] + [block],
        out_specs=(
            pl.BlockSpec((BLOCK, 512), lambda i: (0, 0)),
            block,
            pl.BlockSpec((32, 2, DQK), lambda i: (0, 0, 0)),
            pl.BlockSpec((2, 32), lambda i: (0, 0)),
        ),
        scratch_shapes=[
            pltpu.VMEM((2, DQK, BLOCK), bf16),
            pltpu.VMEM((2, BLOCK, DV), bf16),
            pltpu.VMEM((2, 32, DQK), f32),
            pltpu.VMEM((2, BLOCK, DQK), f32),
            pltpu.VMEM((2, BLOCK, DV), f32),
            pltpu.VMEM((2, BLOCK, DQK), f32),
        ],
        compiler_params=pltpu.CompilerParams(dimension_semantics=("arbitrary",)),
        cost_estimate=pl.CostEstimate(flops=2 * 2048 * 256 * 64, bytes_accessed=17_000_000, transcendentals=0),
        name="cell",
    )(bias, *small, state)
    return hidden, new_matrix, new_normal, new_stable.T


def output_kernel(
    hidden_ref, w_ref, out_ref, gathered, part, mine, got, total, m1, m2, m3, r1, r2, r3, ssem, rsem, psem, qsem, xssem, xrsem
):
    rings = {a: ring_of(a) for a in ("z", "y", "x")}
    core = lax.axis_index("c")
    other = 1 - core
    meet([{a: rings[a][k]} for a in ("z", "y", "x") for k in (1, 2)] + [{"c": other}])
    zme, yme = rings["z"][0], rings["y"][0]
    gathered[zme, yme] = hidden_ref[...]
    sent = []
    arrived = {}
    counter = [0]
    cols = (slice(0, 256), slice(256, 512))

    def ship(key, lane, stage, way, z, y, lo, hi):
        axis = (("z", "y"), ("y", "z"))[lane][stage]
        ref = gathered.at[z, y, lo:hi, cols[lane]]
        slot = counter[0]
        counter[0] += 1
        copy = send(ref, ref, ssem.at[slot], rsem.at[slot], {axis: rings[axis][1 + way]})
        sent.append(copy)
        arrived[key] = copy

    def spot(lane, first, second):
        return (first, second) if lane == 0 else (second, first)

    firsts = (rings["z"], rings["y"])
    seconds = (rings["y"], rings["z"])
    half = BLOCK // 2
    for lane in range(2):
        z, y = spot(lane, firsts[lane][0], seconds[lane][0])
        for way in range(2):
            ship((lane, "a", way), lane, 0, way, z, y, 0, BLOCK)
    for lane in range(2):
        z, y = spot(lane, firsts[lane][0], seconds[lane][0])
        for way in range(2):
            ship((lane, "own", way), lane, 1, way, z, y, 0, BLOCK)
    for lane in range(2):
        me, nxt, prv, opp = firsts[lane]
        second = seconds[lane][0]
        for way, source in ((0, prv), (1, nxt)):
            arrived[(lane, "a", way)].wait_recv()
            z, y = spot(lane, source, second)
            lo, hi = (0, half) if way == 0 else (half, BLOCK)
            ship((lane, "b", way), lane, 0, way, z, y, lo, hi)
            for w in range(2):
                ship((lane, "near", way, w), lane, 1, w, z, y, 0, BLOCK)
    for lane in range(2):
        me, nxt, prv, opp = firsts[lane]
        sme, snxt, sprv, sopp = seconds[lane]
        for way in range(2):
            arrived[(lane, "b", way)].wait_recv()
        z, y = spot(lane, opp, sme)
        for w in range(2):
            ship((lane, "far", w), lane, 1, w, z, y, 0, BLOCK)
        for name, at in (("own", me), (("near", 0), prv), (("near", 1), nxt)):
            for w, source in ((0, sprv), (1, snxt)):
                key = (lane, name, w) if isinstance(name, str) else (lane, *name, w)
                arrived[key].wait_recv()
                z, y = spot(lane, at, source)
                lo, hi = (0, half) if w == 0 else (half, BLOCK)
                ship((lane, "on", name, w), lane, 1, w, z, y, lo, hi)
    for lane in range(2):
        me, nxt, prv, opp = firsts[lane]
        sme, snxt, sprv, sopp = seconds[lane]
        for w, source in ((0, sprv), (1, snxt)):
            arrived[(lane, "far", w)].wait_recv()
            z, y = spot(lane, opp, source)
            lo, hi = (0, half) if w == 0 else (half, BLOCK)
            ship((lane, "on", "far", w), lane, 1, w, z, y, lo, hi)
    for lane in range(2):
        for name in ("own", ("near", 0), ("near", 1), "far"):
            for w in range(2):
                arrived[(lane, "on", name, w)].wait_recv()

    xme, xnxt, xprv, xopp = rings["x"]
    pairs = []
    for group in range(RING):
        z = (xopp, xnxt, xprv, xme)[group]
        rows = gathered[z, pl.ds(2 * other, 2)].reshape(256, 512)
        part[group] = jnp.dot(rows, w_ref[...], preferred_element_type=f32).astype(bf16)
        pairs.append(send(part.at[group], got.at[group], psem.at[group], qsem.at[group], {"c": other}))
    for group in range(RING):
        z = (xopp, xnxt, xprv, xme)[group]
        rows = gathered[z, pl.ds(2 * core, 2)].reshape(256, 512)
        mine[group] = jnp.dot(rows, w_ref[...], preferred_element_type=f32)

    xs = {}

    def ship_x(kind, way, src, dst):
        slot = kind * 2 + way
        xs[(kind, way)] = send(src, dst, xssem.at[slot], xrsem.at[slot], {"x": rings["x"][1 + way]})

    pairs[0].wait_recv()
    total[0] = mine[0] + got[0].astype(f32)
    m1[0] = total[0, :BLOCK].astype(bf16)
    m1[1] = total[0, BLOCK:].astype(bf16)
    ship_x(0, 0, m1.at[0], r1.at[0])
    ship_x(0, 1, m1.at[1], r1.at[1])
    pairs[1].wait_recv()
    total[1] = mine[1] + got[1].astype(f32)
    m2[0] = total[1, BLOCK:].astype(bf16)
    ship_x(1, 0, m2.at[0], r2.at[0])
    pairs[2].wait_recv()
    total[2] = mine[2] + got[2].astype(f32)
    m2[1] = total[2, :BLOCK].astype(bf16)
    ship_x(1, 1, m2.at[1], r2.at[1])
    pairs[3].wait_recv()
    total[3] = mine[3] + got[3].astype(f32)
    xs[(0, 0)].wait_recv()
    m3[0] = (total[1, :BLOCK] + r1[0].astype(f32)).astype(bf16)
    ship_x(2, 0, m3.at[0], r3.at[0])
    xs[(0, 1)].wait_recv()
    m3[1] = (total[2, BLOCK:] + r1[1].astype(f32)).astype(bf16)
    ship_x(2, 1, m3.at[1], r3.at[1])
    for kind in (1, 2):
        for way in range(2):
            xs[(kind, way)].wait_recv()
    out_ref[:BLOCK] = (total[3, :BLOCK] + r3[0].astype(f32) + r2[1].astype(f32)).astype(bf16)
    out_ref[BLOCK:] = (total[3, BLOCK:] + r2[0].astype(f32) + r3[1].astype(f32)).astype(bf16)
    for copy in sent + pairs + list(xs.values()):
        copy.wait_send()


def output(hidden, weight):
    vmem = pl.BlockSpec(memory_space=pltpu.VMEM)
    pair = pltpu.VMEM((2, BLOCK, 256), bf16)
    return pl.pallas_call(
        output_kernel,
        out_shape=jax.ShapeDtypeStruct((256, 256), bf16),
        in_specs=[vmem, vmem],
        out_specs=vmem,
        scratch_shapes=[
            pltpu.VMEM((RING, RING, BLOCK, 512), bf16),
            pltpu.VMEM((RING, 256, 256), bf16),
            pltpu.VMEM((RING, 256, 256), f32),
            pltpu.VMEM((RING, 256, 256), bf16),
            pltpu.VMEM((RING, 256, 256), f32),
            pair, pair, pair, pair, pair, pair,
            pltpu.SemaphoreType.DMA((40,)),
            pltpu.SemaphoreType.DMA((40,)),
            pltpu.SemaphoreType.DMA((4,)),
            pltpu.SemaphoreType.DMA((4,)),
            pltpu.SemaphoreType.DMA((6,)),
            pltpu.SemaphoreType.DMA((6,)),
        ],
        compiler_params=pltpu.CompilerParams(
            collective_id=1, has_side_effects=True, vmem_limit_bytes=40 * 1024 * 1024
        ),
        cost_estimate=pl.CostEstimate(flops=2 * 2048 * 256 * 512, bytes_accessed=3_000_000, transcendentals=0),
        name="output",
    )(hidden, weight)


def per_device(
    tokens, norm_gain, query_weight, key_weight, value_weight, outgate_weight, gate_weight, forget_bias, head_gain,
    output_weight, state_matrix, state_normal, state_stable, prior_keys, prior_values, prior_ingate, prior_forget,
    accepted, parents,
):
    y, g = project(tokens, norm_gain, query_weight, key_weight, value_weight, outgate_weight, gate_weight)
    bias = lax.dynamic_slice_in_dim(forget_bias, lax.axis_index(TP) * 2, 2, 0).reshape(1, 2)
    hidden, new_matrix, new_normal, new_stable = cell(
        y, g, bias, prior_keys, prior_values, prior_ingate, prior_forget, accepted, parents, state_stable, head_gain,
        state_normal, state_matrix,
    )
    layer_out = output(hidden, output_weight)
    return layer_out, new_matrix, new_normal, new_stable


def solution(mesh):
    torus = Mesh(mesh.devices.reshape(4, 4, 4, 2), ("z", "y", "x", "c"))
    placed = (
        P(None, KV), P(), P(KV, TP), P(KV, TP), P(KV, TP), P(KV, TP), P(KV, None), P(), P(TP), P(TP, KV),
        P(KV, TP, None, None), P(KV, TP, None), P(KV, TP), P(KV, None, TP), P(KV, None, TP), P(KV, None, TP),
        P(KV, None, TP), P(KV), P(KV, None),
    )
    return jax.shard_map(
        per_device,
        mesh=torus,
        in_specs=placed,
        out_specs=(P(TP, KV), P(KV, TP, None, None), P(KV, TP, None), P(KV, TP)),
        check_vma=False,
    )
```
